32 devices in a mesh: sp: 4 (over y, x), tp: 8 (over z, core).
Axes of the slice: x: 2, y: 2, z: 4, core: 2. Of those that a mesh axis runs over, the one named last changes fastest.
Arguments:
- queries: bfloat16 [4096, 1024], P('sp', 'tp'), may hold values from -18 to 18
- keys: bfloat16 [4096, 256], P('sp'), may hold values from -18 to 18
- values: bfloat16 [4096, 256], P('sp'), may hold values from -6 to 6
- sink_logits: float32 [16], P('tp'), may hold values from 3 to 7
- w_out: bfloat16 [1024, 2048], P('tp'), may hold values from -1.5 to 1.5
- residual: bfloat16 [4096, 2048], P(('sp', 'tp')), may hold values from -6 to 6
- norm_gain: float32 [2048], replicated, may hold values from 0.1 to 1.9
- expert_ids: int32 [4096, 4], P('sp'), may hold values from 0 to 15, all different within a row; in each aligned block of 1024 rows (0 to 1023, 1024 to 2047, ...) at most 512 rows name the same one
- expert_weights: float32 [4096, 4], P('sp'), may hold values from 0.1 to 1.5
- w_gate: bfloat16 [32, 768, 2048], P(('sp', 'tp')), may hold values from -0.125 to 0.125
- w_up: bfloat16 [32, 768, 2048], P(('sp', 'tp')), may hold values from -0.125 to 0.125
- w_down: bfloat16 [32, 768, 2048], P(('sp', 'tp')), may hold values from -0.15625 to 0.15625
- shared_gate: bfloat16 [512, 2048], P('tp'), may hold values from -0.125 to 0.125
- shared_up: bfloat16 [512, 2048], P('tp'), may hold values from -0.125 to 0.125
- shared_down: bfloat16 [512, 2048], P('tp'), may hold values from -0.25 to 0.25
Outputs:
- layer_out: bfloat16 [4096, 2048], P(('sp', 'tp'))
The draws below stay inside these ranges and needn't reach their ends.
Inputs may be any that keep to these rules, and one draw needn't show every extreme that they name: `expert_ids`: each row names 4 different experts; in each aligned block of 1024 rows no expert is named by more than 512 rows.
All inputs are finite; a program needn't handle non-finite values.
Results may differ from the reference program's by a relative error of at most 0.02.
Values may be sent and summed in bfloat16 or wider, within the bound.
A program may use at most 128 MiB of HBM per device.

```python
import math
import jax
import jax.numpy as jnp
import numpy as np
from jax import lax

D = 2048
HQ = 16
HD = 64
KVH = 4
GROUP = 4
WINDOW = 128
TOK_DEV = 1024
TOKENS = 4096
EXPERTS = 16
TOPK = 4
FF = 1536
SFF = 512
CAP = 512
N_SP = 4
N_TP = 8


def draw_queries(key, part):
    drawn = jnp.clip(jax.random.normal(jax.random.fold_in(key, 11), (TOKENS, HQ * HD), jnp.float32), -6.0, 6.0)
    return drawn.astype(jnp.bfloat16)


def draw_keys(key, part):
    drawn = jnp.clip(jax.random.normal(jax.random.fold_in(key, 23), (TOKENS, KVH * HD), jnp.float32), -6.0, 6.0)
    return drawn.astype(jnp.bfloat16)


def block_levels(key, extent, pieces, low, high):
    def one(dim, blocks):
        heights = jax.random.uniform(jax.random.fold_in(jax.random.fold_in(key, 6), dim), (blocks,), jnp.float32, low / len(pieces), high / len(pieces))
        return jnp.repeat(jnp.exp(heights), extent[dim] // blocks).reshape((-1,) + (1,) * (len(extent) - dim - 1))

    level = one(*pieces[0])
    for cut in pieces[1:]:
        level = level * one(*cut)
    return level


def shared_out(own_key, own, number, rows, count, top, most, slope):
    ranking = jax.random.permutation(own_key, count)
    crowded, common = portions_of(count, rows * top, most, slope, True), portions_of(count, rows * top, most, slope, False)
    places = jnp.arange(count)

    def named(lengths, rotation):
        used = int((lengths > 0).sum())
        fixed = max(1, used // 4)
        shifted = fixed + (places - fixed + rotation * (used - fixed)) % max(1, count - fixed)
        return jnp.zeros((count,), jnp.int32).at[ranking[jnp.where(places < fixed, places, shifted)]].set(jnp.asarray(lengths, jnp.int32))

    lengths = jnp.where(number % 4 == 0, named(crowded, number // 4), named(common, number - number // 4 - 1))
    mixed = jax.random.permutation(jax.random.fold_in(own, 3), count)
    giver, sink = mixed[0:count // 2 * 2:2], mixed[1:count // 2 * 2:2]
    room = jnp.minimum(lengths[giver] - 1, most - lengths[sink]) // 2
    room = jnp.where((giver == ranking[0]) | (sink == ranking[0]) | (lengths[sink] == 0), 0, jnp.maximum(room, 0))
    shifted = jax.random.randint(jax.random.fold_in(own, 4), (count // 2,), 0, 1 << 20) % (room + 1)
    lengths = lengths.at[giver].add(-shifted).at[sink].add(shifted)
    items = jnp.searchsorted(jnp.cumsum(lengths), jnp.arange(rows * top), side="right").astype(jnp.int32)
    listing = items.reshape(top, rows).T
    listing = listing[jax.random.permutation(jax.random.fold_in(own, 1), rows)]
    rotation = jax.random.randint(jax.random.fold_in(own, 2), (rows, 1), 0, top)
    return jnp.take_along_axis(listing, (jnp.arange(top)[None, :] + rotation) % top, axis=1)


def portions_of(amount, total, reach, skew, full):
    portions = [(1 << 20) // math.isqrt(standing ** skew) + 1 for standing in range(1, amount + 1)]
    largest = reach if full else min(reach, max(-(-total // amount), total * portions[0] // sum(portions)))
    least = 1 if total - largest >= amount - 1 else 0
    counts, spare = [largest] + [least] * (amount - 1), total - largest - least * (amount - 1)
    while spare > 0:
        candidates = [i for i in range(1, amount) if counts[i] < largest] or [i for i in range(1, amount) if counts[i] < reach]
        pool, budget = sum([portions[i] for i in candidates]), spare
        for i in candidates:
            addition = min(reach - counts[i], max(1, budget * portions[i] // pool), spare)
            counts[i] = counts[i] + addition
            spare = spare - addition
    return np.array(counts)


def normal_values(rng, shape, width, most, split=(), held_as=jnp.bfloat16):
    gain = block_levels(rng, shape, split, -0.22, 0.18) if split else 1.0
    values = jax.random.normal(rng, shape, jnp.float32) * width * gain
    return jnp.minimum(jnp.maximum(values, -most), most).astype(held_as)


def setup_inputs(seed: int = 0) -> dict:
    key_of = jax.random.split(jax.random.key(seed), 16)
    queries = draw_queries(jax.random.fold_in(key_of[15], 71), 0)
    keys = draw_keys(jax.random.fold_in(key_of[15], 71), 0)
    values = normal_values(key_of[2], (TOKENS, KVH * HD), 1.0, 6.0, ((0, 4),))
    sink_logits = jnp.clip(3.0 + 4.0 * jax.random.uniform(key_of[3], (HQ,), jnp.float32) ** block_levels(key_of[3], (HQ,), ((0, 8),), -0.2, 0.2), 3.0, 7.0)
    w_out = normal_values(key_of[4], (HQ * HD, D), (HQ * HD // 64) ** -0.5, 1.5, ((0, 8),))
    residual = normal_values(key_of[5], (TOKENS, D), 1.0, 6.0, ((0, 32),))
    norm_gain = jnp.clip(1.0 + 0.18 * jax.random.normal(key_of[6], (D,), jnp.float32), 0.1, 1.9)
    expert_ids_keys = jax.random.split(jax.random.fold_in(key_of[7], 1), TOKENS // TOK_DEV)
    expert_ids_turns = jax.random.permutation(jax.random.fold_in(key_of[7], 3), TOKENS // TOK_DEV)
    expert_ids = jax.vmap(lambda own, number: shared_out(jax.random.fold_in(key_of[7], 2), own, number, TOK_DEV, EXPERTS, TOPK, CAP, 2))(expert_ids_keys, expert_ids_turns).reshape((TOKENS, TOPK))
    expert_weights = jnp.clip(jnp.exp(math.log(1.5) - 2.7080502 * jax.random.uniform(key_of[8], (TOKENS, TOPK), jnp.float32) ** block_levels(key_of[8], (TOKENS, TOPK), ((0, 4),), -0.2, 0.2)), 0.1, 1.5)
    w_gate = normal_values(key_of[9], (2 * EXPERTS, FF // 2, D), D ** -0.5, 0.125, ((0, 32),))
    w_up = normal_values(key_of[10], (2 * EXPERTS, FF // 2, D), D ** -0.5, 0.125, ((0, 32),))
    w_down = normal_values(key_of[11], (2 * EXPERTS, FF // 2, D), FF ** -0.5, 0.15625, ((0, 32),))
    shared_gate = normal_values(key_of[12], (SFF, D), D ** -0.5, 0.125, ((0, 8),))
    shared_up = normal_values(key_of[13], (SFF, D), D ** -0.5, 0.125, ((0, 8),))
    shared_down = normal_values(key_of[14], (SFF, D), SFF ** -0.5, 0.25, ((0, 8),))
    return dict(queries=queries, keys=keys, values=values, sink_logits=sink_logits, w_out=w_out, residual=residual, norm_gain=norm_gain, expert_ids=expert_ids, expert_weights=expert_weights, w_gate=w_gate, w_up=w_up, w_down=w_down, shared_gate=shared_gate, shared_up=shared_up, shared_down=shared_down)


def attend(queries, keys, values, sink_logits):
    seq_rows = queries.shape[0]
    num_blocks = seq_rows // WINDOW
    query_blocks = queries.astype(jnp.float32).reshape(num_blocks, WINDOW, KVH, GROUP, HD)
    key_blocks = keys.astype(jnp.float32).reshape(num_blocks, WINDOW, KVH, HD)
    value_blocks = values.astype(jnp.float32).reshape(num_blocks, WINDOW, KVH, HD)

    def shift_back(blocks):
        return jnp.concatenate([jnp.zeros_like(blocks[:1]), blocks[:-1]], axis=0)
    keys_ext = jnp.concatenate([shift_back(key_blocks), key_blocks], axis=1)
    values_ext = jnp.concatenate([shift_back(value_blocks), value_blocks], axis=1)
    scores = jnp.einsum('nqhgd,nshd->nhgqs', query_blocks, keys_ext) * HD ** (-0.5)
    query_pos = jnp.arange(WINDOW)[:, None] + WINDOW
    key_pos = jnp.arange(2 * WINDOW)[None, :]
    in_band = (key_pos <= query_pos) & (key_pos > query_pos - WINDOW)
    absolute = jnp.arange(num_blocks)[:, None, None] * WINDOW + key_pos[None] - WINDOW
    allowed = in_band[None] & (absolute >= 0)
    scores = jnp.where(allowed[:, None, None], scores, -jnp.inf)
    sink_col = jnp.broadcast_to(sink_logits.reshape(KVH, GROUP)[None, :, :, None, None], scores.shape[:-1] + (1,))
    combined = jnp.concatenate([scores, sink_col], axis=-1)
    row_max = lax.optimization_barrier(jnp.max(combined, axis=-1, keepdims=True))
    exps = jnp.exp(combined - row_max)
    weights = (exps[..., :-1] / lax.optimization_barrier(jnp.sum(exps, axis=-1, keepdims=True))).astype(jnp.bfloat16)
    attended = jnp.einsum('nhgqs,nshd->nqhgd', weights.astype(jnp.float32), values_ext)
    return attended.astype(jnp.bfloat16).reshape(seq_rows, HQ * HD)

def normalize(after_mix, norm_gain):
    values_f = after_mix.astype(jnp.float32)
    scale = lax.rsqrt(lax.optimization_barrier(jnp.mean(values_f * values_f, axis=-1, keepdims=True)) + 1e-06)
    return (values_f * scale * norm_gain).astype(jnp.bfloat16)

def slot_layout(route_ids):
    flat_ids = route_ids.reshape(-1).astype(jnp.int32)
    matches = (flat_ids[:, None] == jnp.arange(EXPERTS, dtype=jnp.int32)[None, :]).astype(jnp.int32)
    earlier = jnp.cumsum(matches, axis=0).astype(jnp.int32) - matches
    order_in = lax.optimization_barrier(jnp.sum(earlier * matches, axis=1)).astype(jnp.int32)
    slot_index = flat_ids * CAP + order_in
    owners = jnp.arange(flat_ids.shape[0], dtype=jnp.int32) // TOPK
    slot_owner = jnp.full((EXPERTS * CAP,), -1, jnp.int32).at[slot_index].set(owners)
    return (slot_index, slot_owner)

def run_expert(operands):
    row_block, gate_w, up_w, down_w = operands
    total = jnp.zeros((row_block.shape[0], D), jnp.float32)
    for half in range(2):
        gate_act = jnp.dot(row_block, gate_w[half].T, preferred_element_type=jnp.float32)
        up_act = jnp.dot(row_block, up_w[half].T, preferred_element_type=jnp.float32)
        hidden = (jax.nn.silu(gate_act) * up_act).astype(jnp.bfloat16)
        term = jnp.dot(hidden, down_w[half], preferred_element_type=jnp.float32).astype(jnp.bfloat16)
        term = lax.optimization_barrier(term)
        total = total + term.astype(jnp.float32)
    return total.astype(jnp.bfloat16)

def reference(queries, keys, values, sink_logits, w_out, residual, norm_gain, expert_ids, expert_weights, w_gate, w_up, w_down, shared_gate, shared_up, shared_down):
    attended = attend(queries, keys, values, sink_logits)
    projected = jnp.dot(attended, w_out, preferred_element_type=jnp.float32)
    after_mix = (residual.astype(jnp.float32) + projected).astype(jnp.bfloat16)
    normed = normalize(after_mix, norm_gain)
    block_rows = normed.reshape(N_SP, TOK_DEV, D)
    block_ids = expert_ids.reshape(N_SP, TOK_DEV, TOPK)
    slot_index, slot_owner = jax.vmap(slot_layout)(block_ids)

    def fill_slots(rows_here, owner_here):
        picked = rows_here[jnp.maximum(owner_here, 0)]
        return jnp.where((owner_here >= 0)[:, None], picked, jnp.zeros((), jnp.bfloat16))
    slot_rows = jax.vmap(fill_slots)(block_rows, slot_owner)
    per_expert = jnp.transpose(slot_rows.reshape(N_SP, EXPERTS, CAP, D), (1, 0, 2, 3)).reshape(EXPERTS, N_SP * CAP, D)
    gate_pieces = w_gate.reshape(EXPERTS, 2, FF // 2, D)
    up_pieces = w_up.reshape(EXPERTS, 2, FF // 2, D)
    down_pieces = w_down.reshape(EXPERTS, 2, FF // 2, D)
    expert_out = lax.map(run_expert, (per_expert, gate_pieces, up_pieces, down_pieces))
    returned = jnp.transpose(expert_out.reshape(EXPERTS, N_SP, CAP, D), (1, 0, 2, 3)).reshape(N_SP, EXPERTS * CAP, D)
    shared_hidden = (jax.nn.silu(jnp.dot(normed, shared_gate.T, preferred_element_type=jnp.float32)) * jnp.dot(normed, shared_up.T, preferred_element_type=jnp.float32)).astype(jnp.bfloat16)
    lanes = N_TP // 2
    half_cap = CAP // 2
    unit_width = SFF // N_TP

    def block_moe(operands):
        outputs, index_flat, ids, wts, hidden_rows = operands
        index_pairs = index_flat.reshape(TOK_DEV, TOPK)
        rank = index_pairs - ids * CAP
        group = 2 * (ids % lanes) + rank // half_cap
        chosen = [outputs[index_pairs[:, k]].astype(jnp.float32) for k in range(TOPK)]

        def add_group(total, group_id):
            part = jnp.zeros((TOK_DEV, D), jnp.float32)
            for k in range(TOPK):
                factor = jnp.where(group[:, k] == group_id, wts[:, k], jnp.zeros((), wts.dtype))
                part = part + factor[:, None] * chosen[k]
            hid = lax.dynamic_slice_in_dim(hidden_rows, group_id * unit_width, unit_width, 1)
            down = lax.dynamic_slice_in_dim(shared_down, group_id * unit_width, unit_width, 0)
            part = part + jnp.dot(hid, down, preferred_element_type=jnp.float32)
            rounded = lax.optimization_barrier(part.astype(jnp.bfloat16))
            return (total + rounded.astype(jnp.float32), None)
        total, _ = lax.scan(add_group, jnp.zeros((TOK_DEV, D), jnp.float32), jnp.arange(N_TP, dtype=jnp.int32))
        return total.astype(jnp.bfloat16)
    moe_out = lax.map(block_moe, (returned, slot_index, block_ids, expert_weights.reshape(N_SP, TOK_DEV, TOPK), shared_hidden.reshape(N_SP, TOK_DEV, SFF)))
    moe_out = moe_out.reshape(TOKENS, D)
    return (after_mix.astype(jnp.float32) + moe_out.astype(jnp.float32)).astype(jnp.bfloat16)
```

```python
import jax
import jax.numpy as jnp
from jax import lax
from jax.sharding import PartitionSpec as P

HD = 64
GROUP = 4
WINDOW = 128
TOPK = 4
CHUNKS = 2


def shifted(block, axis, distance):
    devices = range(lax.axis_size(axis))
    route = [(i - distance, i) for i in devices if i - distance in devices]
    return lax.ppermute(block, axis, route)


def from_partner(x, axis, apart):
    return lax.ppermute(x, axis, [(i, i ^ 1 << apart) for i in range(lax.axis_size(axis))])


def normalize(after_mix, norm_gain):
    values_f = after_mix.astype(jnp.float32)
    scale = lax.rsqrt(jnp.mean(values_f * values_f, axis=-1, keepdims=True) + 1e-06)
    return (values_f * scale * norm_gain).astype(jnp.bfloat16)


def lane_slots(route_ids, route_weights, targets, first_rank, half_cap):
    named = route_ids[:, :, None] == targets[None, None, :]
    named_f = jnp.sum(named.astype(jnp.float32), axis=1)
    weight = jnp.sum(jnp.where(named, route_weights[:, :, None], 0.0), axis=1)
    rows = route_ids.shape[0]
    before = jnp.arange(rows)[:, None] > jnp.arange(rows)[None, :]
    rank = jnp.dot(
        before.astype(jnp.bfloat16),
        named_f.astype(jnp.bfloat16),
        preferred_element_type=jnp.float32,
    )
    place = jnp.where(named_f > 0, rank - first_rank, -1.0)
    slots = jnp.arange(half_cap, dtype=jnp.float32)
    picks, mixes = [], []
    for s in range(targets.shape[0]):
        hit = place[:, s : s + 1] == slots[None, :]
        picks.append(jnp.where(hit, 1.0, 0.0).astype(jnp.bfloat16))
        mixes.append(jnp.where(hit, weight[:, s : s + 1], 0.0).astype(jnp.bfloat16))
    return jnp.concatenate(picks, axis=1), jnp.concatenate(mixes, axis=1)


def body(
    queries,
    keys,
    values,
    sink_logits,
    w_out,
    residual,
    norm_gain,
    expert_ids,
    expert_weights,
    w_gate,
    w_up,
    w_down,
    shared_gate,
    shared_up,
    shared_down,
):
    other_gate, other_up, other_down = (from_partner(w[0], "tp", 0) for w in (w_gate, w_up, w_down))
    tp_count = lax.axis_size("tp")
    sp_count = lax.axis_size("sp")
    seq_rows = queries.shape[0]
    expert_count = sp_count * tp_count // 2
    capacity = max(2, 2 * seq_rows * TOPK // expert_count)
    local_heads = queries.shape[1] // HD
    kv_start = lax.axis_index("tp") * local_heads // GROUP * HD
    key_cols = lax.dynamic_slice_in_dim(keys, kv_start, HD, 1)
    value_cols = lax.dynamic_slice_in_dim(values, kv_start, HD, 1)
    rim = jnp.concatenate([keys[seq_rows - WINDOW :], values[seq_rows - WINDOW :]], axis=1)
    rim = shifted(rim, "sp", 1)
    rim_keys = lax.dynamic_slice_in_dim(rim, kv_start, HD, 1)
    rim_values = lax.dynamic_slice_in_dim(rim, kv_start + keys.shape[1], HD, 1)
    num_blocks = seq_rows // WINDOW
    key_blocks = key_cols.reshape(num_blocks, WINDOW, HD)
    value_blocks = value_cols.reshape(num_blocks, WINDOW, HD)
    keys_ext = jnp.concatenate(
        [jnp.concatenate([rim_keys[None], key_blocks[:-1]], axis=0), key_blocks], axis=1
    )
    values_ext = jnp.concatenate(
        [jnp.concatenate([rim_values[None], value_blocks[:-1]], axis=0), value_blocks], axis=1
    )
    query_blocks = queries.reshape(num_blocks, WINDOW, local_heads, HD)
    scores = jnp.einsum(
        "nqhd,nsd->nhqs", query_blocks, keys_ext, preferred_element_type=jnp.float32
    ) * HD ** (-0.5)
    query_pos = jnp.arange(WINDOW)[:, None] + WINDOW
    key_pos = jnp.arange(2 * WINDOW)[None, :]
    in_band = (key_pos <= query_pos) & (key_pos > query_pos - WINDOW)
    absolute = (
        lax.axis_index("sp") * seq_rows
        + jnp.arange(num_blocks)[:, None, None] * WINDOW
        + key_pos[None]
        - WINDOW
    )
    allowed = in_band[None] & (absolute >= 0)
    scores = jnp.where(allowed[:, None], scores, -jnp.inf)
    sink_col = jnp.broadcast_to(sink_logits[None, :, None, None], scores.shape[:-1] + (1,))
    combined = jnp.concatenate([scores, sink_col], axis=-1)
    row_max = jnp.max(combined, axis=-1, keepdims=True)
    exps = jnp.exp(combined - row_max)
    weights = (exps[..., :-1] / jnp.sum(exps, axis=-1, keepdims=True)).astype(jnp.bfloat16)
    attended = jnp.einsum("nhqs,nsd->nqhd", weights, values_ext, preferred_element_type=jnp.float32)
    attended = attended.astype(jnp.bfloat16).reshape(seq_rows, local_heads * HD)
    head_rows = lax.all_to_all(attended, "tp", split_axis=0, concat_axis=1, tiled=True)
    projected = jnp.dot(
        head_rows,
        lax.all_gather(w_out, "tp", axis=0, tiled=True),
        preferred_element_type=jnp.float32,
    )
    after_mix = (residual.astype(jnp.float32) + projected).astype(jnp.bfloat16)
    normed = normalize(after_mix, norm_gain)
    tp_index = lax.axis_index("tp")
    lanes = tp_count // 2
    lane = tp_index // 2
    keep = tp_index % 2
    half_cap = capacity // 2
    targets = jnp.arange(sp_count, dtype=jnp.int32) * lanes + lane
    first_rank = (keep * half_cap).astype(jnp.float32)
    pick, mix = lane_slots(expert_ids, expert_weights, targets, first_rank, half_cap)
    width = after_mix.shape[1]
    step = width // CHUNKS
    gates = [(w_gate[0], w_up[0]), (other_gate, other_up)]
    downs = [w_down[0], other_down]
    sums = [[0.0, 0.0] for _ in gates]
    shared = [0.0, 0.0]
    for c in range(CHUNKS):
        cols = slice(c * step, (c + 1) * step)
        rows = lax.all_gather(normed[:, cols], "tp", axis=0, tiled=True)
        outgoing = lax.dot_general(
            pick, rows, (((0,), (0,)), ((), ())), preferred_element_type=jnp.bfloat16
        )
        arrived = lax.all_to_all(
            outgoing.reshape(sp_count, half_cap, step), "sp", split_axis=0, concat_axis=0, tiled=True
        ).reshape(sp_count * half_cap, step)
        for total, pair in zip(sums, gates):
            for n, w in enumerate(pair):
                total[n] = total[n] + jnp.einsum(
                    "td,fd->tf", arrived, w[:, cols], preferred_element_type=jnp.float32
                )
        for n, w in enumerate((shared_gate, shared_up)):
            shared[n] = shared[n] + jnp.einsum(
                "td,fd->tf", rows, w[:, cols], preferred_element_type=jnp.float32
            )
    shared_hidden = (jax.nn.silu(shared[0]) * shared[1]).astype(jnp.bfloat16)
    hidden = [(jax.nn.silu(g) * u).astype(jnp.bfloat16) for g, u in sums]
    pieces = []
    for c in range(CHUNKS):
        cols = slice(c * step, (c + 1) * step)
        expert_out = sum(
            jnp.dot(h, w[:, cols], preferred_element_type=jnp.float32) for h, w in zip(hidden, downs)
        ).astype(jnp.bfloat16)
        held = lax.all_to_all(
            expert_out.reshape(sp_count, half_cap, step),
            "sp",
            split_axis=0,
            concat_axis=0,
            tiled=True,
        ).reshape(sp_count * half_cap, step)
        part = jnp.dot(shared_hidden, shared_down[:, cols], preferred_element_type=jnp.float32)
        part = part + jnp.dot(mix, held, preferred_element_type=jnp.float32)
        pieces.append(
            lax.psum_scatter(part.astype(jnp.bfloat16), "tp", scatter_dimension=0, tiled=True)
        )
    moe_sum = jnp.concatenate(pieces, axis=1)
    return (after_mix.astype(jnp.float32) + moe_sum.astype(jnp.float32)).astype(jnp.bfloat16)


def solution(mesh):
    return jax.shard_map(
        body,
        mesh=mesh,
        in_specs=(
            P("sp", "tp"),
            P("sp", None),
            P("sp", None),
            P("tp"),
            P("tp", None),
            P(("sp", "tp"), None),
            P(),
            P("sp", None),
            P("sp", None),
            P(("sp", "tp"), None, None),
            P(("sp", "tp"), None, None),
            P(("sp", "tp"), None, None),
            P("tp", None),
            P("tp", None),
            P("tp", None),
        ),
        out_specs=P(("sp", "tp"), None),
        check_vma=False,
    )
```

```python
import jax
import jax.numpy as jnp
from jax import lax
from jax.sharding import PartitionSpec as P

HD = 64
GROUP = 4
WINDOW = 128
TOPK = 4
CHUNKS = 2


def shifted(block, axis, distance):
    devices = range(lax.axis_size(axis))
    route = [(i - distance, i) for i in devices if i - distance in devices]
    return lax.ppermute(block, axis, route)


def from_partner(x, axis, apart):
    return lax.ppermute(x, axis, [(i, i ^ 1 << apart) for i in range(lax.axis_size(axis))])


def normalize(after_mix, norm_gain):
    values_f = after_mix.astype(jnp.float32)
    scale = lax.rsqrt(jnp.mean(values_f * values_f, axis=-1, keepdims=True) + 1e-06)
    return (values_f * scale * norm_gain).astype(jnp.bfloat16)


def lane_slots(route_ids, route_weights, targets, first_rank, half_cap):
    named = route_ids[:, :, None] == targets[None, None, :]
    named_f = jnp.sum(named.astype(jnp.float32), axis=1)
    weight = jnp.sum(jnp.where(named, route_weights[:, :, None], 0.0), axis=1)
    named_t = jnp.sum((route_ids.T[None] == targets[:, None, None]).astype(jnp.float32), axis=1)
    rows = route_ids.shape[0]
    steps = jnp.arange(rows)
    earlier = (steps[None, :] < steps[:, None]).astype(jnp.bfloat16)
    rank = jnp.dot(earlier, named_f.astype(jnp.bfloat16), preferred_element_type=jnp.float32)
    rank_t = jnp.einsum(
        "sq,pq->sp", named_t.astype(jnp.bfloat16), earlier, preferred_element_type=jnp.float32
    )
    place = jnp.where(named_f > 0, rank - first_rank, -1.0)
    place_t = jnp.where(named_t > 0, rank_t - first_rank, -1.0)
    slots = jnp.arange(half_cap, dtype=jnp.float32)
    picks, mixes = [], []
    for s in range(targets.shape[0]):
        hit_t = place_t[s : s + 1, :] == slots[:, None]
        picks.append(jnp.where(hit_t, 1.0, 0.0).astype(jnp.bfloat16))
        hit = place[:, s : s + 1] == slots[None, :]
        mixes.append(jnp.where(hit, weight[:, s : s + 1], 0.0).astype(jnp.bfloat16))
    return jnp.concatenate(picks, axis=0), jnp.concatenate(mixes, axis=1)


def body(
    queries,
    keys,
    values,
    sink_logits,
    w_out,
    residual,
    norm_gain,
    expert_ids,
    expert_weights,
    w_gate,
    w_up,
    w_down,
    shared_gate,
    shared_up,
    shared_down,
):
    other_gate, other_up, other_down = (from_partner(w[0], "tp", 0) for w in (w_gate, w_up, w_down))
    tp_count = lax.axis_size("tp")
    sp_count = lax.axis_size("sp")
    seq_rows = queries.shape[0]
    expert_count = sp_count * tp_count // 2
    capacity = max(2, 2 * seq_rows * TOPK // expert_count)
    local_heads = queries.shape[1] // HD
    kv_start = lax.axis_index("tp") * local_heads // GROUP * HD
    key_cols = lax.dynamic_slice_in_dim(keys, kv_start, HD, 1)
    value_cols = lax.dynamic_slice_in_dim(values, kv_start, HD, 1)
    rim = jnp.concatenate([keys[seq_rows - WINDOW :], values[seq_rows - WINDOW :]], axis=1)
    rim = shifted(rim, "sp", 1)
    rim_keys = lax.dynamic_slice_in_dim(rim, kv_start, HD, 1)
    rim_values = lax.dynamic_slice_in_dim(rim, kv_start + keys.shape[1], HD, 1)
    num_blocks = seq_rows // WINDOW
    key_blocks = key_cols.reshape(num_blocks, WINDOW, HD)
    value_blocks = value_cols.reshape(num_blocks, WINDOW, HD)
    keys_ext = jnp.concatenate(
        [jnp.concatenate([rim_keys[None], key_blocks[:-1]], axis=0), key_blocks], axis=1
    )
    values_ext = jnp.concatenate(
        [jnp.concatenate([rim_values[None], value_blocks[:-1]], axis=0), value_blocks], axis=1
    )
    query_blocks = queries.reshape(num_blocks, WINDOW, local_heads, HD)
    scores = jnp.einsum(
        "nqhd,nsd->nhqs", query_blocks, keys_ext, preferred_element_type=jnp.float32
    ) * HD ** (-0.5)
    query_pos = jnp.arange(WINDOW)[:, None] + WINDOW
    key_pos = jnp.arange(2 * WINDOW)[None, :]
    in_band = (key_pos <= query_pos) & (key_pos > query_pos - WINDOW)
    absolute = (
        lax.axis_index("sp") * seq_rows
        + jnp.arange(num_blocks)[:, None, None] * WINDOW
        + key_pos[None]
        - WINDOW
    )
    allowed = in_band[None] & (absolute >= 0)
    scores = jnp.where(allowed[:, None], scores, -jnp.inf)
    sink_col = jnp.broadcast_to(sink_logits[None, :, None, None], scores.shape[:-1] + (1,))
    combined = jnp.concatenate([scores, sink_col], axis=-1)
    row_max = jnp.max(combined, axis=-1, keepdims=True)
    exps = jnp.exp(combined - row_max)
    weights = (exps[..., :-1] / jnp.sum(exps, axis=-1, keepdims=True)).astype(jnp.bfloat16)
    attended = jnp.einsum("nhqs,nsd->nqhd", weights, values_ext, preferred_element_type=jnp.float32)
    attended = attended.astype(jnp.bfloat16).reshape(seq_rows, local_heads * HD)
    head_rows = lax.all_to_all(attended, "tp", split_axis=0, concat_axis=1, tiled=True)
    head_rows, other_gate, other_up, other_down = lax.optimization_barrier(
        (head_rows, other_gate, other_up, other_down)
    )
    projected = jnp.dot(
        head_rows,
        lax.all_gather(w_out, "tp", axis=0, tiled=True),
        preferred_element_type=jnp.float32,
    )
    after_mix = (residual.astype(jnp.float32) + projected).astype(jnp.bfloat16)
    normed = normalize(after_mix, norm_gain)
    tp_index = lax.axis_index("tp")
    lanes = tp_count // 2
    lane = tp_index // 2
    keep = tp_index % 2
    half_cap = capacity // 2
    targets = jnp.arange(sp_count, dtype=jnp.int32) * lanes + lane
    first_rank = (keep * half_cap).astype(jnp.float32)
    pick, mix = lane_slots(expert_ids, expert_weights, targets, first_rank, half_cap)
    width = after_mix.shape[1]
    step = width // CHUNKS
    gates = [(w_gate[0], w_up[0]), (other_gate, other_up)]
    downs = [w_down[0], other_down]
    sums = [[0.0, 0.0] for _ in gates]
    shared = [0.0, 0.0]
    for c in range(CHUNKS):
        cols = slice(c * step, (c + 1) * step)
        rows = lax.all_gather(normed[:, cols], "tp", axis=0, tiled=True)
        outgoing = jnp.dot(pick, rows, preferred_element_type=jnp.float32).astype(jnp.bfloat16)
        arrived = lax.all_to_all(
            outgoing.reshape(sp_count, half_cap, step), "sp", split_axis=0, concat_axis=0, tiled=True
        ).reshape(sp_count * half_cap, step)
        for total, pair in zip(sums, gates):
            for n, w in enumerate(pair):
                total[n] = total[n] + jnp.einsum(
                    "td,fd->tf", arrived, w[:, cols], preferred_element_type=jnp.float32
                )
        for n, w in enumerate((shared_gate, shared_up)):
            shared[n] = shared[n] + jnp.einsum(
                "td,fd->tf", rows, w[:, cols], preferred_element_type=jnp.float32
            )
    shared_hidden = (jax.nn.silu(shared[0]) * shared[1]).astype(jnp.bfloat16)
    hidden = [(jax.nn.silu(g) * u).astype(jnp.bfloat16) for g, u in sums]
    pieces = []
    outs = []
    for c in range(CHUNKS):
        cols = slice(c * step, (c + 1) * step)
        expert_out = sum(
            jnp.dot(h, w[:, cols], preferred_element_type=jnp.float32) for h, w in zip(hidden, downs)
        ).astype(jnp.bfloat16)
        outs.append(expert_out.reshape(sp_count, half_cap, step))
    for c in range(CHUNKS):
        cols = slice(c * step, (c + 1) * step)
        held = lax.all_to_all(outs[c], "sp", split_axis=0, concat_axis=0, tiled=True)
        if c + 1 < CHUNKS:
            held, outs[c + 1] = lax.optimization_barrier((held, outs[c + 1]))
        held = held.reshape(sp_count * half_cap, step)
        part = jnp.dot(shared_hidden, shared_down[:, cols], preferred_element_type=jnp.float32)
        part = part + jnp.dot(mix, held, preferred_element_type=jnp.float32)
        pieces.append(
            lax.psum_scatter(part.astype(jnp.bfloat16), "tp", scatter_dimension=0, tiled=True)
        )
    moe_sum = jnp.concatenate(pieces, axis=1)
    return (after_mix.astype(jnp.float32) + moe_sum.astype(jnp.float32)).astype(jnp.bfloat16)


def solution(mesh):
    return jax.shard_map(
        body,
        mesh=mesh,
        in_specs=(
            P("sp", "tp"),
            P("sp", None),
            P("sp", None),
            P("tp"),
            P("tp", None),
            P(("sp", "tp"), None),
            P(),
            P("sp", None),
            P("sp", None),
            P(("sp", "tp"), None, None),
            P(("sp", "tp"), None, None),
            P(("sp", "tp"), None, None),
            P("tp", None),
            P("tp", None),
            P("tp", None),
        ),
        out_specs=P(("sp", "tp"), None),
        check_vma=False,
    )
```
